512 devices in a mesh: kv: 64 (over z, y), tp: 8 (over x, core).
Axes of the slice: x: 4, y: 4, z: 16, core: 2. Of those that a mesh axis runs over, the one named last changes fastest.
Arguments:
- tokens: bfloat16 [64, 4096], P(None, 'kv'), may hold values from -160 to 160
- norm_gain: float32 [4096], P('kv'), may hold values from 0.1 to 1.9
- w_query: bfloat16 [4096, 2048], P('kv', 'tp'), may hold values from -0.09375 to 0.09375
- w_key: bfloat16 [4096, 2048], P('kv', 'tp'), may hold values from -0.5 to 0.5
- w_value: bfloat16 [4096, 2048], P('kv', 'tp'), may hold values from -0.09375 to 0.09375
- w_out: bfloat16 [2048, 4096], P('tp', 'kv'), may hold values from -0.125 to 0.125
- lambdas: float32 [16], P('tp'), may hold values from 0.3 to 0.8
- sub_gain: float32 [128], replicated, may hold values from 0.1 to 1.9
- key_cache: bfloat16 [4, 16, 32768, 128], P(None, 'tp', 'kv'), may hold values from -512 to 512
- value_cache: bfloat16 [4, 16, 32768, 128], P(None, 'tp', 'kv'), may hold values from -6 to 6
- prior: int32 [4], replicated, may hold values from 24576 to 32736
- accepted: int32 [4], replicated, may hold values from 1 to 16
- parent: int32 [4, 16], replicated, may hold values from -1 to 14, as said below
Outputs:
- mixed: bfloat16 [64, 4096], P('tp', 'kv')
- key_out: bfloat16 [4, 16, 32768, 128], P(None, 'tp', 'kv')
- value_out: bfloat16 [4, 16, 32768, 128], P(None, 'tp', 'kv')
The draws below stay inside these ranges and needn't reach their ends.
Inputs may be any that keep to these rules, and one draw needn't show every extreme that they name: parent[s, 0] is -1, and 0 <= parent[s, j] < j for j >= 1.
All inputs are finite; a program needn't handle non-finite values.
Results may differ from the reference program's by a relative error of at most 0.015.
The reference program's roundings to bfloat16 on the way count: a program that leaves them out, or rounds other values in their place, can miss the bound.
Values may be sent and summed in bfloat16 or wider, within the bound.
A program may use at most 64 MiB of HBM per device.

```python
import jax
import jax.numpy as jnp
from jax import lax

D = 4096
HEADS = 16
HDIM = 64
VDIM = 128
SEQS = 4
PROPS = 16
CTX = 32768
TOKENS = 64
N_TP = 8


def draw_tokens(key, part):
    columns = jnp.arange(D, dtype=jnp.float32) / D
    row_power = jax.random.uniform(jax.random.fold_in(key, 3), (TOKENS, 1), jnp.float32, 0.0, 1.0)
    base = jnp.clip(jax.random.normal(jax.random.fold_in(key, 5), (TOKENS, D), jnp.float32), -4.0, 4.0)
    rising = 3.0 ** columns
    return (base * rising[None, :] * 10.0 ** row_power).astype(jnp.bfloat16)


def draw_key_cache(key, part):
    shape = (SEQS, HEADS, CTX, 2 * HDIM)
    base = 1.75 * jnp.clip(jax.random.normal(jax.random.fold_in(key, 7), shape, jnp.float32), -6.0, 6.0)
    return base.astype(jnp.bfloat16)


def draw_parent(key, part):
    offsets = jax.random.randint(jax.random.fold_in(key, 11), (SEQS, PROPS), 1, 5)
    positions = jnp.arange(PROPS, dtype=jnp.int32)[None, :]
    chosen = jnp.maximum(positions - offsets, 0)
    return jnp.where(positions == 0, -1, chosen).astype(jnp.int32)


def place_ends(values, key, smallest, largest):
    extent = values.shape
    index_at = [jax.random.randint(jax.random.fold_in(key, axis), (), 0, extent[axis]) for axis in range(len(extent))]
    values = values.at[tuple(index_at)].set(smallest)
    longest = extent.index(max(extent))
    index_at[longest] = (index_at[longest] + 1) % extent[longest]
    return values.at[tuple(index_at)].set(largest)


def shard_levels(own_key, dims, split, smallest, high):
    def one(axis_at, parts):
        draws = jax.random.uniform(jax.random.fold_in(jax.random.fold_in(own_key, 6), axis_at), (parts,), jnp.float32, smallest / len(split), high / len(split))
        return jnp.repeat(jnp.exp(draws), dims[axis_at] // parts).reshape((-1,) + (1,) * (len(dims) - axis_at - 1))

    level = one(*split[0])
    for cut in split[1:]:
        level = level * one(*cut)
    return level


def centred(rng, extent, scale, limit, cuts=(), held_as=jnp.bfloat16):
    gain = shard_levels(rng, extent, cuts, -0.22, 0.18) if cuts else 1.0
    result = jax.random.normal(rng, extent, jnp.float32) * scale * gain
    return jnp.minimum(jnp.maximum(result, -limit), limit).astype(held_as)


def setup_inputs(seed: int = 0) -> dict:
    splits = jax.random.split(jax.random.key(seed), 14)
    tokens = draw_tokens(jax.random.fold_in(splits[13], 71), 0)
    norm_gain = jnp.clip(1.0 + 0.18 * jax.random.normal(splits[1], (D,), jnp.float32), 0.1, 1.9)
    w_query = centred(splits[2], (D, HEADS * 2 * HDIM), D ** -0.5, 0.09375, ((0, 64), (1, 8)))
    w_key = centred(splits[3], (D, HEADS * 2 * HDIM), (D // 32) ** -0.5, 0.5, ((0, 64), (1, 8)))
    w_value = centred(splits[4], (D, HEADS * VDIM), D ** -0.5, 0.09375, ((0, 64), (1, 8)))
    w_out = centred(splits[5], (HEADS * VDIM, D), (HEADS * VDIM) ** -0.5, 0.125, ((0, 8), (1, 64)))
    lambdas = jnp.clip(0.3 + 0.5 * jax.random.uniform(splits[6], (HEADS,), jnp.float32) ** shard_levels(splits[6], (HEADS,), ((0, 8),), -0.2, 0.2), 0.3, 0.8)
    sub_gain = jnp.clip(1.0 + 0.18 * jax.random.normal(splits[7], (VDIM,), jnp.float32), 0.1, 1.9)
    key_cache = draw_key_cache(jax.random.fold_in(splits[13], 71), 0)
    value_cache = centred(splits[9], (SEQS, HEADS, CTX, VDIM), 1.0, 6.0, ((1, 8), (2, 64)))
    prior = place_ends(jax.random.randint(splits[10], (SEQS,), CTX * 3 // 4, CTX - 2 * PROPS + 1), jax.random.fold_in(splits[10], 1), CTX * 3 // 4, CTX - 2 * PROPS).astype(jnp.int32)
    accepted = place_ends(jax.random.randint(splits[11], (SEQS,), 1, PROPS + 1), jax.random.fold_in(splits[11], 1), 1, PROPS).astype(jnp.int32)
    parent = draw_parent(jax.random.fold_in(splits[13], 71), 0)
    return dict(tokens=tokens, norm_gain=norm_gain, w_query=w_query, w_key=w_key, w_value=w_value, w_out=w_out, lambdas=lambdas, sub_gain=sub_gain, key_cache=key_cache, value_cache=value_cache, prior=prior, accepted=accepted, parent=parent)


epsilon = 1e-06
masked_score = -1e+30
head_scale = 0.8

def ancestors(parent):
    prop_count = parent.shape[1]
    identity = jnp.eye(prop_count, dtype=jnp.float32)
    parent_hot = (parent[:, :, None] == jnp.arange(prop_count, dtype=jnp.int32)[None, None, :]).astype(jnp.float32)

    def extend(depth_step, ancestry):
        return identity[None] + jnp.einsum('sjm,smi->sji', parent_hot, ancestry, precision=lax.Precision.HIGHEST)
    return lax.fori_loop(0, prop_count, extend, jnp.broadcast_to(identity, parent_hot.shape))

def reference(tokens, norm_gain, w_query, w_key, w_value, w_out, lambdas, sub_gain, key_cache, value_cache, prior, accepted, parent):
    as_float = tokens.astype(jnp.float32)
    row_scale = lax.rsqrt(lax.optimization_barrier(jnp.mean(as_float * as_float, axis=1)) + epsilon)
    normed = (as_float * norm_gain[None, :]).astype(jnp.bfloat16)

    def project(weight_matrix):
        product = jnp.dot(normed, weight_matrix, preferred_element_type=jnp.float32)
        return (row_scale[:, None] * product).astype(jnp.bfloat16)
    queries = project(w_query).reshape(SEQS, PROPS, HEADS, 2, HDIM)
    new_key = project(w_key).reshape(SEQS, PROPS, HEADS, 2 * HDIM).transpose(0, 2, 1, 3)
    new_value = project(w_value).reshape(SEQS, PROPS, HEADS, VDIM).transpose(0, 2, 1, 3)
    valid_end = (prior + accepted).astype(jnp.int32)
    zero_index = jnp.int32(0)

    def write_rows(cache_seq, rows_seq, start):
        return lax.dynamic_update_slice(cache_seq, rows_seq, (zero_index, start.astype(jnp.int32), zero_index))
    key_out = jax.vmap(write_rows)(key_cache, new_key, valid_end)
    value_out = jax.vmap(write_rows)(value_cache, new_value, valid_end)
    ancestry = ancestors(parent)
    positions = jnp.arange(CTX, dtype=jnp.int32)
    prop_iota = jnp.arange(PROPS, dtype=jnp.int32)

    def attend_one(item):
        query_seq, keys_seq, values_seq, valid_seq, ancestry_seq = item
        offset_in = positions - valid_seq
        one_hot = (offset_in[:, None] == prop_iota[None, :]).astype(jnp.float32)
        in_tree = jnp.dot(ancestry_seq, one_hot.T, precision=lax.Precision.HIGHEST)
        allowed = (offset_in < 0)[None, :] | (in_tree > 0.5)
        visible = allowed[None, None]
        halves = keys_seq.astype(jnp.float32).reshape(HEADS, CTX, 2, HDIM)
        scores = jnp.einsum('jhmd,hpmd->mhjp', query_seq.astype(jnp.float32), halves) * HDIM ** (-0.5)
        maximum = lax.optimization_barrier(jnp.max(jnp.where(visible, scores, masked_score), axis=-1, keepdims=True))
        weight = jnp.where(visible, jnp.exp(scores - maximum), 0.0)
        totals = lax.optimization_barrier(jnp.sum(weight, axis=-1))
        rounded = lax.optimization_barrier(weight.astype(jnp.bfloat16)).astype(jnp.float32)
        summed = jnp.einsum('mhjp,hpc->mhjc', rounded, values_seq.astype(jnp.float32))
        head_out = summed[0] / totals[0][..., None] - lambdas[:, None, None] * summed[1] / totals[1][..., None]
        mean_square = lax.optimization_barrier(jnp.mean(head_out * head_out, axis=-1, keepdims=True))
        normed_head = head_out * lax.rsqrt(mean_square + epsilon) * sub_gain * head_scale
        return normed_head.transpose(1, 0, 2).astype(jnp.bfloat16)
    attended = lax.map(attend_one, (queries, key_out, value_out, valid_end, ancestry))
    group_size = HEADS // N_TP * VDIM
    attended = attended.reshape(TOKENS, N_TP, group_size)
    out_groups = w_out.reshape(N_TP, group_size, D)
    partial_value = jnp.einsum('tgc,gcd->gtd', attended.astype(jnp.float32), out_groups.astype(jnp.float32))
    partial_value = lax.optimization_barrier(partial_value.astype(jnp.bfloat16)).astype(jnp.float32)
    mixed = lax.optimization_barrier(jnp.sum(partial_value, axis=0)).astype(jnp.bfloat16)
    return (mixed, key_out, value_out)
```

```python
import functools

import jax
import jax.numpy as jnp
from jax import lax
from jax.experimental import pallas as pl
from jax.experimental.pallas import tpu as pltpu
from jax.sharding import PartitionSpec as P

MESH = pl.DeviceIdType.MESH
VMEM = pl.BlockSpec(memory_space=pltpu.VMEM)
SMEM = pl.BlockSpec(memory_space=pltpu.SMEM)
HBM = pl.BlockSpec(memory_space=pl.ANY)

D = 4096
NZ, NY, NT = 16, 4, 8
SEQS, PROPS, TOKENS = 4, 16, 64
EPS = 1e-06
MASKED = -1e30
HEAD_SCALE = 0.8
F32, BF16 = jnp.float32, jnp.bfloat16


def z_step(k):
    odd = lax.rem(k, 2)
    return 8 + odd * lax.div(k + 1, 2) - (1 - odd) * lax.div(k, 2)


def to_plane(z, y, tp, send):
    def far(i, carry):
        tz = lax.rem(z + z_step(lax.div(i, NY)), NZ)
        ty = lax.rem(y + lax.rem(i, NY), NY)
        send(tz, ty)
        return carry

    lax.fori_loop(0, (NZ - 1) * NY, far, 0)

    def near(i, carry):
        send(z, lax.rem(y + i, NY))
        return carry

    lax.fori_loop(1, NY, near, 0)


def wait_bytes(ref, count, sem):
    piece = ref.at[pl.ds(0, count)]
    pltpu.make_async_copy(piece, piece, sem).wait()


def split3(x):
    high = x.astype(BF16).astype(F32)
    rest = x - high
    mid = rest.astype(BF16).astype(F32)
    return high, mid, (rest - mid).astype(BF16).astype(F32)


def fused(
    tok_ref, gain_ref, wq_ref, wk_ref, wv_ref, wo_ref, lam_ref, sub_ref, prior_ref, acc_ref, par_ref, kc_ref, vc_ref,
    mixed_ref, nk_ref, nv_ref,
    kbuf, vbuf, part, yb, zsrc, zb, ag, rows, terms, csrc, cb, cterms, att, attf, psrc, pb,
    load_sem, y_send, y_recv, z_send, z_recv, a_send, a_recv, c_send, c_recv, t_send, t_recv, p_send, p_recv,
):
    kv, tp = lax.axis_index("kv"), lax.axis_index("tp")
    z, y = lax.div(kv, NY), lax.rem(kv, NY)
    mine = y * NZ + z
    length = kbuf.shape[2]

    load_k = pltpu.make_async_copy(kc_ref, kbuf, load_sem.at[0])
    load_v = pltpu.make_async_copy(vc_ref, vbuf, load_sem.at[1])

    barrier = pltpu.get_barrier_semaphore()

    def greet(tz, ty):
        pl.semaphore_signal(barrier, inc=1, device_id=(tz * NY + ty, tp), device_id_type=MESH)

    to_plane(z, y, tp, greet)

    def greet_tp(i, carry):
        pl.semaphore_signal(barrier, inc=1, device_id=(kv, lax.rem(tp + i, NT)), device_id_type=MESH)
        return carry

    lax.fori_loop(1, NT, greet_tp, 0)
    load_k.start()
    load_v.start()

    x = tok_ref[...].astype(F32)
    normed = (x * gain_ref[...]).astype(BF16)
    squares = jnp.sum(x * x, axis=1, keepdims=True)
    for c, w in enumerate((wq_ref, wk_ref, wv_ref)):
        product = jnp.dot(normed, w[...], preferred_element_type=F32)
        part[:, 2 * c, :] = product[:, :128]
        part[:, 2 * c + 1, :] = product[:, 128:]
    part[:, 6, :] = jnp.broadcast_to(squares, (TOKENS, 128))

    at_i = lax.broadcasted_iota(jnp.int32, (PROPS, PROPS), 0)
    at_j = lax.broadcasted_iota(jnp.int32, (PROPS, PROPS), 1)
    twice_j = lax.rem(lax.broadcasted_iota(jnp.int32, (2 * PROPS, PROPS), 0), PROPS)
    twice_i = lax.broadcasted_iota(jnp.int32, (2 * PROPS, PROPS), 1)
    twice = jnp.where(twice_j == twice_i, 1.0, 0.0).astype(BF16)
    ancestry = []
    for s in range(SEQS):
        parents = par_ref[s : s + 1, :]
        reach = jnp.where((at_i == parents) | (at_i == at_j), 1.0, 0.0)
        for _ in range(4):
            step = reach.astype(BF16)
            reach = jnp.where(jnp.dot(step, step, preferred_element_type=F32) > 0.5, 1.0, 0.0)
        ancestry.append(
            lax.dot_general(twice, reach.astype(BF16), (((1,), (1,)), ((), ())), preferred_element_type=F32)
        )

    pl.semaphore_wait(barrier, NZ * NY - 1 + NT - 1)

    for step in (2, 1, 3):
        ty = lax.rem(y + step, NY)
        pltpu.make_async_remote_copy(
            part.at[pl.ds(ty * NZ, NZ)], yb.at[y], y_send, y_recv, device_id=(z * NY + ty, tp), device_id_type=MESH
        ).start()
    yb[y] = part[pl.ds(y * NZ, NZ)]
    wait_bytes(yb, NY - 1, y_recv)
    zsrc[...] = (yb[0] + yb[1]) + (yb[2] + yb[3])

    def send_z(k, carry):
        tz = lax.rem(z + z_step(k), NZ)
        pltpu.make_async_remote_copy(
            zsrc.at[tz], zb.at[z], z_send, z_recv, device_id=(tz * NY + y, tp), device_id_type=MESH
        ).start()
        return carry

    lax.fori_loop(0, NZ - 1, send_z, 0)
    zb[z] = zsrc[z]
    wait_bytes(zb, NZ - 1, z_recv)
    total = jnp.sum(zb[...], axis=0)
    scale = lax.rsqrt(total[6:7, :] / D + EPS)
    ag[mine] = (total[:6, :] * scale).astype(BF16)

    def send_a(tz, ty):
        pltpu.make_async_remote_copy(
            ag.at[mine], ag.at[mine], a_send, a_recv, device_id=(tz * NY + ty, tp), device_id_type=MESH
        ).start()

    to_plane(z, y, tp, send_a)
    load_k.wait()
    load_v.wait()
    wait_bytes(ag, NZ * NY - 1, a_recv)
    rows[...] = ag[...].astype(F32)

    base = kv * length
    lane = lax.broadcasted_iota(jnp.int32, (PROPS, 128), 1)
    position = lax.broadcasted_iota(jnp.int32, (2 * PROPS, length), 1) + base
    tree_at = lax.broadcasted_iota(jnp.int32, (2 * PROPS, PROPS), 1) - base
    contract_last = (((1,), (1,)), ((), ()))
    for s in range(SEQS):
        end = prior_ref[s] + acc_ref[s]
        settled = position < end
        placed = tree_at + end
        in_tree = (ancestry[s] > 0.5) & (placed >= 0) & (placed < length)
        tokens = slice(s * PROPS, (s + 1) * PROPS)
        stats = jnp.zeros((PROPS, 128), F32)
        for h in range(2):
            q = rows[tokens, h, :]
            both = jnp.concatenate([jnp.where(lane < 64, q, 0.0), jnp.where(lane < 64, 0.0, q)], axis=0).astype(BF16)
            new_k = rows[tokens, 2 + h, :].astype(BF16)
            new_v = rows[tokens, 4 + h, :].astype(BF16)
            nk_ref[s, h] = new_k
            nv_ref[s, h] = new_v
            scores = lax.dot_general(both, kbuf[s, h], contract_last, preferred_element_type=F32) * 0.125
            tree = lax.dot_general(both, new_k, contract_last, preferred_element_type=F32) * 0.125
            maximum = jnp.maximum(
                jnp.max(jnp.where(settled, scores, MASKED), axis=1, keepdims=True),
                jnp.max(jnp.where(in_tree, tree, MASKED), axis=1, keepdims=True),
            )
            weight = jnp.where(settled, jnp.exp(scores - maximum), 0.0)
            tree_weight = jnp.where(in_tree, jnp.exp(tree - maximum), 0.0)
            totals = jnp.sum(weight, axis=1, keepdims=True) + jnp.sum(tree_weight, axis=1, keepdims=True)
            summed = jnp.dot(weight.astype(BF16), vbuf[s, h], preferred_element_type=F32) + jnp.dot(
                tree_weight.astype(BF16), new_v, preferred_element_type=F32
            )
            for m in range(2):
                c = 2 * m + h
                half = slice(m * PROPS, (m + 1) * PROPS)
                terms[tokens, c, :] = summed[half]
                for n, column in ((c, maximum[half]), (4 + c, totals[half])):
                    for k, piece in enumerate(split3(column)):
                        stats = jnp.where(lane == 8 * k + n, piece, stats)
        terms[tokens, 4, :] = stats
        terms[tokens, 5, :] = jnp.zeros((PROPS, 128), F32)
    csrc[...] = terms[...].astype(BF16)

    def send_c(tz, ty):
        pltpu.make_async_remote_copy(
            csrc.at[ty * NZ + tz], cb.at[mine], c_send, c_recv, device_id=(tz * NY + ty, tp), device_id_type=MESH
        ).start()

    to_plane(z, y, tp, send_c)
    cb[mine] = csrc[mine]
    wait_bytes(cb, NZ * NY - 1, c_recv)
    cterms[...] = cb[...].astype(F32)

    st = cterms[:, 4, :]
    heads = []
    for c in range(4):
        maxima = (st[:, c : c + 1] + st[:, 8 + c : 9 + c]) + st[:, 16 + c : 17 + c]
        shares = (st[:, 4 + c : 5 + c] + st[:, 12 + c : 13 + c]) + st[:, 20 + c : 21 + c]
        factor = jnp.exp(maxima - jnp.max(maxima, axis=0, keepdims=True))
        whole = jnp.sum(factor * shares, axis=0, keepdims=True)
        heads.append(jnp.sum(factor * cterms[:, c, :], axis=0, keepdims=True) / whole)
    attended = []
    for h in range(2):
        head_out = heads[h] - lam_ref[h] * heads[2 + h]
        square = jnp.mean(head_out * head_out, axis=1, keepdims=True)
        attended.append(head_out * lax.rsqrt(square + EPS) * sub_ref[...] * HEAD_SCALE)
    att[mine] = jnp.concatenate(attended, axis=0).astype(BF16)

    def send_t(tz, ty):
        pltpu.make_async_remote_copy(
            att.at[mine], att.at[mine], t_send, t_recv, device_id=(tz * NY + ty, tp), device_id_type=MESH
        ).start()

    to_plane(z, y, tp, send_t)
    psrc[...] = jnp.zeros(psrc.shape, F32)
    wait_bytes(att, NZ * NY - 1, t_recv)
    attf[...] = att[...].astype(F32)

    out = jnp.dot(attf[:, 0, :].astype(BF16), wo_ref[:128, :], preferred_element_type=F32) + jnp.dot(
        attf[:, 1, :].astype(BF16), wo_ref[128:, :], preferred_element_type=F32
    )
    psrc[:, :, :64] = out.astype(BF16).astype(F32).reshape(NT, TOKENS // NT, 64)

    def send_p(i, carry):
        other = lax.rem(tp + i, NT)
        pltpu.make_async_remote_copy(
            psrc.at[other], pb.at[tp], p_send, p_recv, device_id=(kv, other), device_id_type=MESH
        ).start()
        return carry

    lax.fori_loop(1, NT, send_p, 0)
    pb[tp] = psrc[tp]
    wait_bytes(yb, NY - 1, y_send)
    wait_bytes(zb, NZ - 1, z_send)
    wait_bytes(ag, NZ * NY - 1, a_send)
    wait_bytes(cb, NZ * NY - 1, c_send)
    wait_bytes(att, NZ * NY - 1, t_send)
    wait_bytes(pb, NT - 1, p_recv)
    wait_bytes(pb, NT - 1, p_send)
    mixed_ref[...] = jnp.sum(pb[...], axis=0)[:, :64].astype(BF16)


def insert(prior_ref, acc_ref, nk_ref, nv_ref, k_ref, v_ref, ko_ref, vo_ref):
    s = pl.program_id(0)
    length = k_ref.shape[2]
    end = prior_ref[s] + acc_ref[s] - lax.axis_index("kv") * length
    offset = lax.broadcasted_iota(jnp.int32, (length, PROPS), 0) - end
    hot = jnp.where(offset == lax.broadcasted_iota(jnp.int32, (length, PROPS), 1), 1.0, 0.0).astype(BF16)
    across = lax.broadcasted_iota(jnp.int32, (length, 128), 0) - end
    inside = (across >= 0) & (across < PROPS)
    for new, old, out in ((nk_ref, k_ref, ko_ref), (nv_ref, v_ref, vo_ref)):
        for h in range(2):
            placed = jnp.dot(hot, new[0, h], preferred_element_type=F32)
            out[0, h] = jnp.where(inside, placed, old[0, h].astype(F32)).astype(BF16)


def body(
    tokens, norm_gain, w_query, w_key, w_value, w_out, lambdas, sub_gain, key_cache, value_cache, prior, accepted, parent
):
    length = key_cache.shape[2]
    new_rows = jax.ShapeDtypeStruct((SEQS, 2, PROPS, 128), BF16)
    mixed, new_key, new_value = pl.pallas_call(
        fused,
        name="fused",
        out_shape=(jax.ShapeDtypeStruct((TOKENS // NT, 64), BF16), new_rows, new_rows),
        in_specs=[VMEM] * 6 + [SMEM, VMEM, SMEM, SMEM, VMEM, HBM, HBM],
        out_specs=(VMEM,) * 3,
        scratch_shapes=[
            pltpu.VMEM((SEQS, 2, length, 128), BF16),
            pltpu.VMEM((SEQS, 2, length, 128), BF16),
            pltpu.VMEM((TOKENS, 7, 128), F32),
            pltpu.VMEM((NY, NZ, 7, 128), F32),
            pltpu.VMEM((NZ, 7, 128), F32),
            pltpu.VMEM((NZ, 7, 128), F32),
            pltpu.VMEM((TOKENS, 6, 128), BF16),
            pltpu.VMEM((TOKENS, 6, 128), F32),
            pltpu.VMEM((TOKENS, 6, 128), F32),
            pltpu.VMEM((TOKENS, 6, 128), BF16),
            pltpu.VMEM((TOKENS, 6, 128), BF16),
            pltpu.VMEM((TOKENS, 6, 128), F32),
            pltpu.VMEM((TOKENS, 2, 128), BF16),
            pltpu.VMEM((TOKENS, 2, 128), F32),
            pltpu.VMEM((NT, TOKENS // NT, 128), F32),
            pltpu.VMEM((NT, TOKENS // NT, 128), F32),
            pltpu.SemaphoreType.DMA((2,)),
        ]
        + [pltpu.SemaphoreType.DMA] * 12,
        compiler_params=pltpu.CompilerParams(collective_id=0, has_side_effects=True),
    )(
        tokens, norm_gain.reshape(1, -1), w_query, w_key, w_value, w_out, lambdas, sub_gain.reshape(1, -1),
        prior, accepted, parent, key_cache, value_cache,
    )
    rows = pl.BlockSpec((1, 2, PROPS, 128), lambda s: (s, 0, 0, 0))
    shard = pl.BlockSpec((1, 2, length, 128), lambda s: (s, 0, 0, 0))
    cache = jax.ShapeDtypeStruct(key_cache.shape, BF16)
    key_out, value_out = pl.pallas_call(
        insert,
        name="insert",
        grid=(SEQS,),
        out_shape=(cache, cache),
        in_specs=[SMEM, SMEM, rows, rows, shard, shard],
        out_specs=(shard, shard),
    )(prior, accepted, new_key, new_value, key_cache, value_cache)
    return mixed, key_out, value_out


def solution(mesh):
    in_specs = (
        P(None, "kv"),
        P("kv"),
        P("kv", "tp"),
        P("kv", "tp"),
        P("kv", "tp"),
        P("tp", "kv"),
        P("tp"),
        P(),
        P(None, "tp", "kv", None),
        P(None, "tp", "kv", None),
        P(),
        P(),
        P(),
    )
    out_specs = (P("tp", "kv"), P(None, "tp", "kv", None), P(None, "tp", "kv", None))
    return jax.shard_map(body, mesh=mesh, in_specs=in_specs, out_specs=out_specs, check_vma=False)
```

```python
import functools

import jax
import jax.numpy as jnp
from jax import lax
from jax.experimental import pallas as pl
from jax.experimental.pallas import tpu as pltpu
from jax.sharding import PartitionSpec as P

MESH = pl.DeviceIdType.MESH
HBM = pl.BlockSpec(memory_space=pl.ANY)
VMEM = pl.BlockSpec(memory_space=pltpu.VMEM)

D = 4096
NZ, NY, NT = 16, 4, 8
HALF = NZ // 2
SEQS, PROPS, TOKENS = 4, 16, 64
EPS = 1e-06
MASKED = -1e30
HEAD_SCALE = 0.8
F32, BF16 = jnp.float32, jnp.bfloat16
LAST = (((1,), (1,)), ((), ()))
OUT = pltpu.VMEM


def z_step(k):
    odd = lax.rem(k, 2)
    return 8 + odd * lax.div(k + 1, 2) - (1 - odd) * lax.div(k, 2)


def half_step(k):
    odd = lax.rem(k, 2)
    return odd * (19 - lax.div(k, 2)) + (1 - odd) * (12 + lax.div(k, 2))


def to_plane(z, y, steps, step_of, send):
    def far(i, carry):
        send(lax.rem(z + step_of(lax.div(i, NY)), NZ), lax.rem(y + lax.rem(i, NY), NY))
        return carry

    lax.fori_loop(0, steps * NY, far, 0)

    def near(i, carry):
        send(z, lax.rem(y + i, NY))
        return carry

    lax.fori_loop(1, NY, near, 0)


def wait_bytes(ref, count, sem):
    piece = ref.at[pl.ds(0, count)]
    pltpu.make_async_copy(piece, piece, sem).wait()


def split3(x):
    high = x.astype(BF16).astype(F32)
    rest = x - high
    mid = rest.astype(BF16).astype(F32)
    return high, mid, (rest - mid).astype(BF16).astype(F32)


def fused(
    tok_in, gain_in, wq_in, wk_in, wv_in, wo_in, lam_in, sub_in, prior_in, acc_in, par_in, kc_in, vc_in,
    mixed_ref, kbuf, vbuf,
    tok, gain, wq, wk, wv, sub, par, lam, prior, acc, woall,
    part_q, part_n, yb_q, yb_n, zs_q, zs_n, zb_q, zb_n, ag_q, ag_n, ruler_q, ruler_n, rows, news, reach_ref,
    terms, csrc, cb, cterms, asrc, attb, attf,
    load_sem, y_send, y_recv, yn_send, yn_recv, w_send, w_recv, z_send, z_recv, zn_send, zn_recv,
    a_send, a_recv, an_send, an_recv, c_send, c_recv, t_send, t_recv,
):
    kv, tp = lax.axis_index("kv"), lax.axis_index("tp")
    z, y = lax.div(kv, NY), lax.rem(kv, NY)
    mine = y * NZ + z
    low, upper = lax.rem(z, HALF), lax.div(z, HALF)
    length = kbuf.shape[2]

    barrier = pltpu.get_barrier_semaphore()

    def greet(tz, ty):
        pl.semaphore_signal(barrier, inc=1, device_id=(tz * NY + ty, tp), device_id_type=MESH)

    to_plane(z, y, NZ - 1, z_step, greet)

    def greet_tp(i, carry):
        pl.semaphore_signal(barrier, inc=1, device_id=(kv, lax.rem(tp + i, NT)), device_id_type=MESH)
        return carry

    lax.fori_loop(1, NT, greet_tp, 0)

    pairs = (
        (tok_in, tok), (gain_in, gain), (wq_in, wq), (wk_in, wk), (wv_in, wv), (par_in, par), (wo_in, woall.at[tp]),
        (sub_in, sub), (lam_in, lam), (prior_in, prior), (acc_in, acc), (kc_in, kbuf), (vc_in, vbuf),
    )
    loads = [pltpu.make_async_copy(a, b, load_sem.at[i]) for i, (a, b) in enumerate(pairs)]
    for load in loads:
        load.start()
    for load in loads[:6]:
        load.wait()

    x = tok[...].astype(F32)
    normed = (x * gain[...]).astype(BF16)
    squares = jnp.sum(x * x, axis=1, keepdims=True)
    for w, out, c in ((wq, part_q, 0), (wk, part_n, 0), (wv, part_n, 2)):
        product = jnp.dot(normed, w[...], preferred_element_type=F32)
        out[:, c, :] = product[:, :128]
        out[:, c + 1, :] = product[:, 128:]
    part_q[:, 2, :] = jnp.broadcast_to(squares, (TOKENS, 128))

    at_i = lax.broadcasted_iota(jnp.int32, (PROPS, PROPS), 0)
    at_j = lax.broadcasted_iota(jnp.int32, (PROPS, PROPS), 1)
    for s in range(SEQS):
        reach = jnp.where((at_i == par[s : s + 1, :]) | (at_i == at_j), 1.0, 0.0)
        for _ in range(4):
            step = reach.astype(BF16)
            reach = jnp.where(jnp.dot(step, step, preferred_element_type=F32) > 0.5, 1.0, 0.0)
        reach_ref[s] = reach

    for load in loads[6:]:
        load.wait()
    pl.semaphore_wait(barrier, NZ * NY - 1 + NT - 1)

    def send_y(part, yb, sends, recvs):
        for step in (2, 1, 3):
            ty = lax.rem(y + step, NY)
            pltpu.make_async_remote_copy(
                part.at[pl.ds(ty * NZ, NZ)], yb.at[y], sends, recvs, device_id=(z * NY + ty, tp), device_id_type=MESH
            ).start()

    def send_z(zs, zb, sends, recvs):
        def one(k, carry):
            tz = lax.rem(z + z_step(k), NZ)
            pltpu.make_async_remote_copy(
                zs.at[:, lax.rem(tz, HALF)], zb.at[z], sends, recvs, device_id=(tz * NY + y, tp), device_id_type=MESH
            ).start()
            return carry

        lax.fori_loop(0, NZ - 1, one, 0)

    def send_rows(ag, sends, recvs):
        def one(tz, ty):
            piece = ag.at[y, :, low]
            pltpu.make_async_remote_copy(
                piece, piece, sends, recvs, device_id=(tz * NY + ty, tp), device_id_type=MESH
            ).start()

        to_plane(z, y, HALF - 1, half_step, one)

    send_y(part_q, yb_q, y_send, y_recv)
    send_y(part_n, yb_n, yn_send, yn_recv)

    def send_w(i, carry):
        pltpu.make_async_remote_copy(
            woall.at[tp], woall.at[tp], w_send, w_recv, device_id=(kv, lax.rem(tp + i, NT)), device_id_type=MESH
        ).start()
        return carry

    lax.fori_loop(1, NT, send_w, 0)

    for part, yb, recvs, zs, zb, z_sends, z_recvs in (
        (part_q, yb_q, y_recv, zs_q, zb_q, z_send, z_recv),
        (part_n, yb_n, yn_recv, zs_n, zb_n, zn_send, zn_recv),
    ):
        yb[y] = part[pl.ds(y * NZ, NZ)]
        wait_bytes(yb, NY - 1, recvs)
        zs[...] = ((yb[0] + yb[1]) + (yb[2] + yb[3])).reshape(zs.shape)
        send_z(zs, zb, z_sends, z_recvs)
        zb[z] = zs[:, low]

    wait_bytes(zb_q, NZ - 1, z_recv)
    total = jnp.sum(zb_q[...], axis=0)
    scale = lax.rsqrt(total[:, 2:3, :] / D + EPS)
    ag_q[y, :, low] = (total[:, :2, :] * scale).astype(BF16)
    send_rows(ag_q, a_send, a_recv)
    wait_bytes(zb_n, NZ - 1, zn_recv)
    ag_n[y, :, low] = (jnp.sum(zb_n[...], axis=0) * scale).astype(BF16)
    send_rows(ag_n, an_send, an_recv)

    wait_bytes(ruler_q, TOKENS - 2, a_recv)
    rows[...] = ag_q[...].astype(F32).reshape(rows.shape)
    lane = lax.broadcasted_iota(jnp.int32, (PROPS, 128), 1)
    position = lax.broadcasted_iota(jnp.int32, (2 * PROPS, length), 1) + kv * length
    for s in range(SEQS):
        settled = position < prior[s] + acc[s]
        tokens = slice(s * PROPS, (s + 1) * PROPS)
        stats = jnp.zeros((PROPS, 128), F32)
        for h in range(2):
            q = rows[tokens, h, :]
            both = jnp.concatenate([jnp.where(lane < 64, q, 0.0), jnp.where(lane < 64, 0.0, q)], axis=0).astype(BF16)
            scores = lax.dot_general(both, kbuf[s, h], LAST, preferred_element_type=F32) * 0.125
            maximum = jnp.max(jnp.where(settled, scores, MASKED), axis=1, keepdims=True)
            weight = jnp.where(settled, jnp.exp(scores - maximum), 0.0)
            totals = jnp.sum(weight, axis=1, keepdims=True)
            summed = jnp.dot(weight.astype(BF16), vbuf[s, h], preferred_element_type=F32)
            for m in range(2):
                c = 2 * m + h
                half = slice(m * PROPS, (m + 1) * PROPS)
                terms[tokens, c, :] = summed[half]
                for n, column in ((c, maximum[half]), (4 + c, totals[half])):
                    for k, piece in enumerate(split3(column)):
                        stats = jnp.where(lane == 8 * k + n, piece, stats)
        terms[tokens, 4, :] = stats
        terms[tokens, 5, :] = jnp.zeros((PROPS, 128), F32)
    csrc[...] = terms[...].astype(BF16)

    def send_c(tz, ty):
        pltpu.make_async_remote_copy(
            csrc.at[ty * NZ + tz], cb.at[mine], c_send, c_recv, device_id=(tz * NY + ty, tp), device_id_type=MESH
        ).start()

    to_plane(z, y, NZ - 1, z_step, send_c)
    cb[mine] = csrc[mine]

    wait_bytes(ruler_n, TOKENS - 2, an_recv)
    news[...] = ag_n[...].astype(F32).reshape(news.shape)
    own_q = ag_q[y, upper, low].astype(F32)
    family = pl.ds(y * PROPS, PROPS)
    related = jnp.sum(jnp.where(at_j == z, reach_ref[y], 0.0), axis=1, keepdims=True) > 0.5
    tree = []
    for m in range(2):
        for h in range(2):
            product = own_q[h : h + 1, :] * news[family, h, :]
            mine_only = lane < 64 if m == 0 else lane >= 64
            scores = jnp.sum(jnp.where(mine_only, product, 0.0), axis=1, keepdims=True) * 0.125
            maximum = jnp.max(jnp.where(related, scores, MASKED), axis=0, keepdims=True)
            weight = jnp.where(related, jnp.exp(scores - maximum), 0.0)
            summed = jnp.sum(weight.astype(BF16).astype(F32) * news[family, 2 + h, :], axis=0, keepdims=True)
            tree.append((maximum, jnp.sum(weight, axis=0, keepdims=True), summed))

    offset = lax.broadcasted_iota(jnp.int32, (length, PROPS), 0) + kv * length
    column = lax.broadcasted_iota(jnp.int32, (length, PROPS), 1)
    across = lax.broadcasted_iota(jnp.int32, (length, 128), 0) + kv * length
    for s in range(SEQS):
        end = prior[s] + acc[s]
        hot = jnp.where(offset - end == column, 1.0, 0.0).astype(BF16)
        inside = (across >= end) & (across < end + PROPS)
        for h in range(2):
            for buf, c in ((kbuf, h), (vbuf, 2 + h)):
                new = news[s * PROPS : (s + 1) * PROPS, c, :].astype(BF16)
                placed = jnp.dot(hot, new, preferred_element_type=F32)
                buf[s, h] = jnp.where(inside, placed, buf[s, h].astype(F32)).astype(BF16)

    wait_bytes(cb, NZ * NY - 1, c_recv)
    cterms[...] = cb[...].astype(F32)
    st = cterms[:, 4, :]
    heads = []
    for c in range(4):
        tree_max, tree_total, tree_summed = tree[c]
        maxima = (st[:, c : c + 1] + st[:, 8 + c : 9 + c]) + st[:, 16 + c : 17 + c]
        shares = (st[:, 4 + c : 5 + c] + st[:, 12 + c : 13 + c]) + st[:, 20 + c : 21 + c]
        largest = jnp.maximum(jnp.max(maxima, axis=0, keepdims=True), tree_max)
        factor, tree_factor = jnp.exp(maxima - largest), jnp.exp(tree_max - largest)
        whole = jnp.sum(factor * shares, axis=0, keepdims=True) + tree_factor * tree_total
        summed = jnp.sum(factor * cterms[:, c, :], axis=0, keepdims=True) + tree_factor * tree_summed
        heads.append(summed / whole)
    attended = []
    for h in range(2):
        head_out = heads[h] - lam[h] * heads[2 + h]
        square = jnp.mean(head_out * head_out, axis=1, keepdims=True)
        attended.append(head_out * lax.rsqrt(square + EPS) * sub[...] * HEAD_SCALE)
    done = jnp.concatenate(attended, axis=0).astype(BF16)
    asrc[...] = done

    target = 2 * y + upper

    def send_t(tz, ty):
        pltpu.make_async_remote_copy(
            asrc, attb.at[tp, low], t_send, t_recv, device_id=(tz * NY + ty, target), device_id_type=MESH
        ).start()

    to_plane(z, y, NZ - 1, z_step, send_t)

    @pl.when(target == tp)
    def _():
        attb[tp, low] = done
        wait_bytes(ruler_q, TOKENS - 1, t_recv)
        wait_bytes(ruler_q, TOKENS - 1, t_send)

    @pl.when(target != tp)
    def _():
        send_t(z, y)
        wait_bytes(ruler_q, TOKENS, t_recv)
        wait_bytes(ruler_q, TOKENS, t_send)

    wait_bytes(woall, NT - 1, w_recv)

    attf[...] = attb[...].astype(F32).reshape(attf.shape)
    mixed = jnp.zeros(mixed_ref.shape, F32)
    for g in range(NT):
        group = slice(g * 8, (g + 1) * 8)
        product = lax.dot_general(
            attf[group, 0, :].astype(BF16), woall[g, :, :128], LAST, preferred_element_type=F32
        ) + lax.dot_general(attf[group, 1, :].astype(BF16), woall[g, :, 128:], LAST, preferred_element_type=F32)
        mixed += product.astype(BF16).astype(F32)
    mixed_ref[...] = mixed.astype(BF16)

    wait_bytes(yb_q, NY - 1, y_send)
    wait_bytes(yb_n, NY - 1, yn_send)
    wait_bytes(woall, NT - 1, w_send)
    wait_bytes(zb_q, NZ - 1, z_send)
    wait_bytes(zb_n, NZ - 1, zn_send)
    wait_bytes(ruler_q, TOKENS - 2, a_send)
    wait_bytes(ruler_n, TOKENS - 2, an_send)
    wait_bytes(cb, NZ * NY - 1, c_send)


def body(
    tokens, norm_gain, w_query, w_key, w_value, w_out, lambdas, sub_gain, key_cache, value_cache, prior, accepted, parent
):
    length = key_cache.shape[2]
    return pl.pallas_call(
        fused,
        name="fused",
        out_shape=(
            OUT((TOKENS // NT, 64), BF16),
            OUT(key_cache.shape, BF16),
            OUT(value_cache.shape, BF16),
        ),
        in_specs=[HBM] * 13,
        out_specs=(VMEM,) * 3,
        scratch_shapes=[
            pltpu.VMEM((TOKENS, 64), BF16),
            pltpu.VMEM((1, 64), F32),
            pltpu.VMEM((64, 256), BF16),
            pltpu.VMEM((64, 256), BF16),
            pltpu.VMEM((64, 256), BF16),
            pltpu.VMEM((1, 128), F32),
            pltpu.VMEM((SEQS, PROPS), jnp.int32),
            pltpu.SMEM((2,), F32),
            pltpu.SMEM((SEQS,), jnp.int32),
            pltpu.SMEM((SEQS,), jnp.int32),
            pltpu.VMEM((NT, 64, 256), BF16),
            pltpu.VMEM((TOKENS, 3, 128), F32),
            pltpu.VMEM((TOKENS, 4, 128), F32),
            pltpu.VMEM((NY, NZ, 3, 128), F32),
            pltpu.VMEM((NY, NZ, 4, 128), F32),
            pltpu.VMEM((2, HALF, 3, 128), F32),
            pltpu.VMEM((2, HALF, 4, 128), F32),
            pltpu.VMEM((NZ, 2, 3, 128), F32),
            pltpu.VMEM((NZ, 2, 4, 128), F32),
            pltpu.VMEM((SEQS, 2, HALF, 2, 128), BF16),
            pltpu.VMEM((SEQS, 2, HALF, 4, 128), BF16),
            pltpu.VMEM((TOKENS, 2, 128), BF16),
            pltpu.VMEM((TOKENS, 4, 128), BF16),
            pltpu.VMEM((TOKENS, 2, 128), F32),
            pltpu.VMEM((TOKENS, 4, 128), F32),
            pltpu.VMEM((SEQS, PROPS, PROPS), F32),
            pltpu.VMEM((TOKENS, 6, 128), F32),
            pltpu.VMEM((TOKENS, 6, 128), BF16),
            pltpu.VMEM((TOKENS, 6, 128), BF16),
            pltpu.VMEM((TOKENS, 6, 128), F32),
            pltpu.VMEM((2, 128), BF16),
            pltpu.VMEM((NT, 8, 2, 128), BF16),
            pltpu.VMEM((TOKENS, 2, 128), F32),
            pltpu.SemaphoreType.DMA((13,)),
        ]
        + [pltpu.SemaphoreType.DMA] * 18,
        compiler_params=pltpu.CompilerParams(collective_id=0, has_side_effects=True),
    )(
        tokens, norm_gain.reshape(1, -1), w_query, w_key, w_value, w_out.T, lambdas, sub_gain.reshape(1, -1),
        prior, accepted, parent, key_cache, value_cache,
    )


def solution(mesh):
    in_specs = (
        P(None, "kv"),
        P("kv"),
        P("kv", "tp"),
        P("kv", "tp"),
        P("kv", "tp"),
        P("tp", "kv"),
        P("tp"),
        P(),
        P(None, "tp", "kv", None),
        P(None, "tp", "kv", None),
        P(),
        P(),
        P(),
    )
    out_specs = (P("tp", "kv"), P(None, "tp", "kv", None), P(None, "tp", "kv", None))
    return jax.shard_map(body, mesh=mesh, in_specs=in_specs, out_specs=out_specs, check_vma=False)
```

```python
import functools

import jax
import jax.numpy as jnp
from jax import lax
from jax.experimental import pallas as pl
from jax.experimental.pallas import tpu as pltpu
from jax.sharding import PartitionSpec as P

MESH = pl.DeviceIdType.MESH
HBM = pl.BlockSpec(memory_space=pl.ANY)
VMEM = pl.BlockSpec(memory_space=pltpu.VMEM)

D = 4096
NZ, NY, NT = 16, 4, 8
HALF = NZ // 2
SEQS, PROPS, TOKENS = 4, 16, 64
EPS = 1e-06
MASKED = -1e30
HEAD_SCALE = 0.8
F32, BF16 = jnp.float32, jnp.bfloat16
LAST = (((1,), (1,)), ((), ()))
OUT = pltpu.VMEM


def z_step(k):
    odd = lax.rem(k, 2)
    return 8 + odd * lax.div(k + 1, 2) - (1 - odd) * lax.div(k, 2)


def half_step(k):
    odd = lax.rem(k, 2)
    return odd * (19 - lax.div(k, 2)) + (1 - odd) * (12 + lax.div(k, 2))


def to_plane(z, y, steps, step_of, send):
    def far(i, carry):
        send(lax.rem(z + step_of(lax.div(i, NY)), NZ), lax.rem(y + lax.rem(i, NY), NY))
        return carry

    lax.fori_loop(0, steps * NY, far, 0)

    def near(i, carry):
        send(z, lax.rem(y + i, NY))
        return carry

    lax.fori_loop(1, NY, near, 0)


def wait_bytes(ref, count, sem):
    piece = ref.at[pl.ds(0, count)]
    pltpu.make_async_copy(piece, piece, sem).wait()


def split3(x):
    high = x.astype(BF16).astype(F32)
    rest = x - high
    mid = rest.astype(BF16).astype(F32)
    return high, mid, (rest - mid).astype(BF16).astype(F32)


def fused(
    tok_in, gain_in, wq_in, wk_in, wv_in, wo_in, lam_in, sub_in, prior_in, acc_in, par_in, kc_in, vc_in,
    mixed_ref, kbuf, vbuf,
    tok, gain, wq, wk, wv, sub, par, lam, prior, acc, woall,
    part_q, part_n, yb_q, yb_n, zs_q, zs_n, zb_q, zb_n, ag_q, ag_n, ruler_q, ruler_n, rows, news, reach_ref,
    terms, csrc, cb, cterms, asrc, attb, attf,
    load_sem, y_send, y_recv, yn_send, yn_recv, w_send, w_recv, z_send, z_recv, zn_send, zn_recv,
    a_send, a_recv, an_send, an_recv, c_send, c_recv, t_send, t_recv, in_2, in_4, in_8,
):
    kv, tp = lax.axis_index("kv"), lax.axis_index("tp")
    z, y = lax.div(kv, NY), lax.rem(kv, NY)
    mine = y * NZ + z
    low, upper = lax.rem(z, HALF), lax.div(z, HALF)
    length = kbuf.shape[2]

    barrier = pltpu.get_barrier_semaphore()

    def signal_z(step, sem):
        for tz in (lax.rem(z + step, NZ), lax.rem(z + NZ - step, NZ)):
            pl.semaphore_signal(sem, inc=1, device_id=(tz * NY + y, tp), device_id_type=MESH)

    signal_z(1, barrier)
    for i in range(1, NY):
        pl.semaphore_signal(barrier, inc=1, device_id=(z * NY + lax.rem(y + i, NY), tp), device_id_type=MESH)
    for i in range(1, NT):
        pl.semaphore_signal(barrier, inc=1, device_id=(kv, lax.rem(tp + i, NT)), device_id_type=MESH)

    pairs = (
        (tok_in, tok), (gain_in, gain), (wq_in, wq), (wk_in, wk), (wv_in, wv), (par_in, par), (wo_in, woall.at[tp]),
        (sub_in, sub), (lam_in, lam), (prior_in, prior), (acc_in, acc), (kc_in, kbuf), (vc_in, vbuf),
    )
    loads = [pltpu.make_async_copy(a, b, load_sem.at[i]) for i, (a, b) in enumerate(pairs)]
    for load in loads:
        load.start()
    for load in loads[:6]:
        load.wait()

    x = tok[...].astype(F32)
    normed = (x * gain[...]).astype(BF16)
    squares = jnp.sum(x * x, axis=1, keepdims=True)
    for w, out, c in ((wq, part_q, 0), (wk, part_n, 0), (wv, part_n, 2)):
        product = jnp.dot(normed, w[...], preferred_element_type=F32)
        out[:, c, :] = product[:, :128]
        out[:, c + 1, :] = product[:, 128:]
    part_q[:, 2, :] = jnp.broadcast_to(squares, (TOKENS, 128))

    at_i = lax.broadcasted_iota(jnp.int32, (PROPS, PROPS), 0)
    at_j = lax.broadcasted_iota(jnp.int32, (PROPS, PROPS), 1)
    for s in range(SEQS):
        reach = jnp.where((at_i == par[s : s + 1, :]) | (at_i == at_j), 1.0, 0.0)
        for _ in range(4):
            step = reach.astype(BF16)
            reach = jnp.where(jnp.dot(step, step, preferred_element_type=F32) > 0.5, 1.0, 0.0)
        reach_ref[s] = reach

    pl.semaphore_wait(barrier, 2 + NY - 1 + NT - 1)
    signal_z(1, in_2)

    def send_y(part, yb, sends, recvs):
        for step in (2, 1, 3):
            ty = lax.rem(y + step, NY)
            pltpu.make_async_remote_copy(
                part.at[pl.ds(ty * NZ, NZ)], yb.at[y], sends, recvs, device_id=(z * NY + ty, tp), device_id_type=MESH
            ).start()

    def send_z(zs, zb, sends, recvs):
        def one(k, carry):
            tz = lax.rem(z + z_step(k), NZ)
            pltpu.make_async_remote_copy(
                zs.at[:, lax.rem(tz, HALF)], zb.at[z], sends, recvs, device_id=(tz * NY + y, tp), device_id_type=MESH
            ).start()
            return carry

        lax.fori_loop(0, NZ - 1, one, 0)

    def send_rows(ag, sends, recvs):
        def one(tz, ty):
            piece = ag.at[y, :, low]
            pltpu.make_async_remote_copy(
                piece, piece, sends, recvs, device_id=(tz * NY + ty, tp), device_id_type=MESH
            ).start()

        to_plane(z, y, HALF - 1, half_step, one)

    send_y(part_q, yb_q, y_send, y_recv)
    send_y(part_n, yb_n, yn_send, yn_recv)

    def send_w(i, carry):
        pltpu.make_async_remote_copy(
            woall.at[tp], woall.at[tp], w_send, w_recv, device_id=(kv, lax.rem(tp + i, NT)), device_id_type=MESH
        ).start()
        return carry

    pl.semaphore_wait(in_2, 2)
    signal_z(2, in_4)
    loads[6].wait()
    lax.fori_loop(1, NT, send_w, 0)
    pl.semaphore_wait(in_4, 2)
    signal_z(4, in_8)
    for load in loads[7:]:
        load.wait()

    for part, yb, recvs, zs, zb, z_sends, z_recvs in (
        (part_q, yb_q, y_recv, zs_q, zb_q, z_send, z_recv),
        (part_n, yb_n, yn_recv, zs_n, zb_n, zn_send, zn_recv),
    ):
        yb[y] = part[pl.ds(y * NZ, NZ)]
        wait_bytes(yb, NY - 1, recvs)
        zs[...] = ((yb[0] + yb[1]) + (yb[2] + yb[3])).reshape(zs.shape)
        if part is part_q:
            pl.semaphore_wait(in_8, 2)
        send_z(zs, zb, z_sends, z_recvs)
        zb[z] = zs[:, low]

    wait_bytes(zb_q, NZ - 1, z_recv)
    total = jnp.sum(zb_q[...], axis=0)
    scale = lax.rsqrt(total[:, 2:3, :] / D + EPS)
    ag_q[y, :, low] = (total[:, :2, :] * scale).astype(BF16)
    send_rows(ag_q, a_send, a_recv)
    wait_bytes(zb_n, NZ - 1, zn_recv)
    ag_n[y, :, low] = (jnp.sum(zb_n[...], axis=0) * scale).astype(BF16)
    send_rows(ag_n, an_send, an_recv)

    wait_bytes(ruler_q, TOKENS - 2, a_recv)
    rows[...] = ag_q[...].astype(F32).reshape(rows.shape)
    lane = lax.broadcasted_iota(jnp.int32, (PROPS, 128), 1)
    position = lax.broadcasted_iota(jnp.int32, (2 * PROPS, length), 1) + kv * length
    for s in range(SEQS):
        settled = position < prior[s] + acc[s]
        tokens = slice(s * PROPS, (s + 1) * PROPS)
        stats = jnp.zeros((PROPS, 128), F32)
        for h in range(2):
            q = rows[tokens, h, :]
            both = jnp.concatenate([jnp.where(lane < 64, q, 0.0), jnp.where(lane < 64, 0.0, q)], axis=0).astype(BF16)
            scores = lax.dot_general(both, kbuf[s, h], LAST, preferred_element_type=F32) * 0.125
            maximum = jnp.max(jnp.where(settled, scores, MASKED), axis=1, keepdims=True)
            weight = jnp.where(settled, jnp.exp(scores - maximum), 0.0)
            totals = jnp.sum(weight, axis=1, keepdims=True)
            summed = jnp.dot(weight.astype(BF16), vbuf[s, h], preferred_element_type=F32)
            for m in range(2):
                c = 2 * m + h
                half = slice(m * PROPS, (m + 1) * PROPS)
                terms[tokens, c, :] = summed[half]
                for n, column in ((c, maximum[half]), (4 + c, totals[half])):
                    for k, piece in enumerate(split3(column)):
                        stats = jnp.where(lane == 8 * k + n, piece, stats)
        terms[tokens, 4, :] = stats
        terms[tokens, 5, :] = jnp.zeros((PROPS, 128), F32)
    csrc[...] = terms[...].astype(BF16)

    def send_c(tz, ty):
        pltpu.make_async_remote_copy(
            csrc.at[ty * NZ + tz], cb.at[mine], c_send, c_recv, device_id=(tz * NY + ty, tp), device_id_type=MESH
        ).start()

    to_plane(z, y, NZ - 1, z_step, send_c)
    cb[mine] = csrc[mine]

    wait_bytes(ruler_n, TOKENS - 2, an_recv)
    news[...] = ag_n[...].astype(F32).reshape(news.shape)
    own_q = ag_q[y, upper, low].astype(F32)
    family = pl.ds(y * PROPS, PROPS)
    related = jnp.sum(jnp.where(at_j == z, reach_ref[y], 0.0), axis=1, keepdims=True) > 0.5
    tree = []
    for m in range(2):
        for h in range(2):
            product = own_q[h : h + 1, :] * news[family, h, :]
            mine_only = lane < 64 if m == 0 else lane >= 64
            scores = jnp.sum(jnp.where(mine_only, product, 0.0), axis=1, keepdims=True) * 0.125
            maximum = jnp.max(jnp.where(related, scores, MASKED), axis=0, keepdims=True)
            weight = jnp.where(related, jnp.exp(scores - maximum), 0.0)
            summed = jnp.sum(weight.astype(BF16).astype(F32) * news[family, 2 + h, :], axis=0, keepdims=True)
            tree.append((maximum, jnp.sum(weight, axis=0, keepdims=True), summed))

    offset = lax.broadcasted_iota(jnp.int32, (length, PROPS), 0) + kv * length
    column = lax.broadcasted_iota(jnp.int32, (length, PROPS), 1)
    across = lax.broadcasted_iota(jnp.int32, (length, 128), 0) + kv * length
    for s in range(SEQS):
        end = prior[s] + acc[s]
        hot = jnp.where(offset - end == column, 1.0, 0.0).astype(BF16)
        inside = (across >= end) & (across < end + PROPS)
        for h in range(2):
            for buf, c in ((kbuf, h), (vbuf, 2 + h)):
                new = news[s * PROPS : (s + 1) * PROPS, c, :].astype(BF16)
                placed = jnp.dot(hot, new, preferred_element_type=F32)
                buf[s, h] = jnp.where(inside, placed, buf[s, h].astype(F32)).astype(BF16)

    wait_bytes(cb, NZ * NY - 1, c_recv)
    cterms[...] = cb[...].astype(F32)
    st = cterms[:, 4, :]
    heads = []
    for c in range(4):
        tree_max, tree_total, tree_summed = tree[c]
        maxima = (st[:, c : c + 1] + st[:, 8 + c : 9 + c]) + st[:, 16 + c : 17 + c]
        shares = (st[:, 4 + c : 5 + c] + st[:, 12 + c : 13 + c]) + st[:, 20 + c : 21 + c]
        largest = jnp.maximum(jnp.max(maxima, axis=0, keepdims=True), tree_max)
        factor, tree_factor = jnp.exp(maxima - largest), jnp.exp(tree_max - largest)
        whole = jnp.sum(factor * shares, axis=0, keepdims=True) + tree_factor * tree_total
        summed = jnp.sum(factor * cterms[:, c, :], axis=0, keepdims=True) + tree_factor * tree_summed
        heads.append(summed / whole)
    attended = []
    for h in range(2):
        head_out = heads[h] - lam[h] * heads[2 + h]
        square = jnp.mean(head_out * head_out, axis=1, keepdims=True)
        attended.append(head_out * lax.rsqrt(square + EPS) * sub[...] * HEAD_SCALE)
    done = jnp.concatenate(attended, axis=0).astype(BF16)
    asrc[...] = done

    target = 2 * y + upper

    def send_t(tz, ty):
        pltpu.make_async_remote_copy(
            asrc, attb.at[tp, low], t_send, t_recv, device_id=(tz * NY + ty, target), device_id_type=MESH
        ).start()

    to_plane(z, y, NZ - 1, z_step, send_t)

    @pl.when(target == tp)
    def _():
        attb[tp, low] = done
        wait_bytes(ruler_q, TOKENS - 1, t_recv)
        wait_bytes(ruler_q, TOKENS - 1, t_send)

    @pl.when(target != tp)
    def _():
        send_t(z, y)
        wait_bytes(ruler_q, TOKENS, t_recv)
        wait_bytes(ruler_q, TOKENS, t_send)

    wait_bytes(woall, NT - 1, w_recv)

    attf[...] = attb[...].astype(F32).reshape(attf.shape)
    mixed = jnp.zeros(mixed_ref.shape, F32)
    for g in range(NT):
        group = slice(g * 8, (g + 1) * 8)
        product = lax.dot_general(
            attf[group, 0, :].astype(BF16), woall[g, :, :128], LAST, preferred_element_type=F32
        ) + lax.dot_general(attf[group, 1, :].astype(BF16), woall[g, :, 128:], LAST, preferred_element_type=F32)
        mixed += product.astype(BF16).astype(F32)
    mixed_ref[...] = mixed.astype(BF16)

    wait_bytes(yb_q, NY - 1, y_send)
    wait_bytes(yb_n, NY - 1, yn_send)
    wait_bytes(woall, NT - 1, w_send)
    wait_bytes(zb_q, NZ - 1, z_send)
    wait_bytes(zb_n, NZ - 1, zn_send)
    wait_bytes(ruler_q, TOKENS - 2, a_send)
    wait_bytes(ruler_n, TOKENS - 2, an_send)
    wait_bytes(cb, NZ * NY - 1, c_send)


def copy_out(mixed_ref, k_ref, v_ref, mixed_out, k_out, v_out, sems):
    copies = [pltpu.make_async_copy(mixed_ref, mixed_out, sems.at[2 * SEQS])]
    for s in range(SEQS):
        copies.append(pltpu.make_async_copy(k_ref.at[s], k_out.at[s], sems.at[s]))
        copies.append(pltpu.make_async_copy(v_ref.at[s], v_out.at[s], sems.at[SEQS + s]))
    for copy in copies:
        copy.start()
    for copy in copies:
        copy.wait()


def body(
    tokens, norm_gain, w_query, w_key, w_value, w_out, lambdas, sub_gain, key_cache, value_cache, prior, accepted, parent
):
    length = key_cache.shape[2]
    results = pl.pallas_call(
        fused,
        name="fused",
        out_shape=(
            OUT((TOKENS // NT, 64), BF16),
            OUT(key_cache.shape, BF16),
            OUT(value_cache.shape, BF16),
        ),
        in_specs=[HBM] * 13,
        out_specs=(VMEM,) * 3,
        scratch_shapes=[
            pltpu.VMEM((TOKENS, 64), BF16),
            pltpu.VMEM((1, 64), F32),
            pltpu.VMEM((64, 256), BF16),
            pltpu.VMEM((64, 256), BF16),
            pltpu.VMEM((64, 256), BF16),
            pltpu.VMEM((1, 128), F32),
            pltpu.VMEM((SEQS, PROPS), jnp.int32),
            pltpu.SMEM((2,), F32),
            pltpu.SMEM((SEQS,), jnp.int32),
            pltpu.SMEM((SEQS,), jnp.int32),
            pltpu.VMEM((NT, 64, 256), BF16),
            pltpu.VMEM((TOKENS, 3, 128), F32),
            pltpu.VMEM((TOKENS, 4, 128), F32),
            pltpu.VMEM((NY, NZ, 3, 128), F32),
            pltpu.VMEM((NY, NZ, 4, 128), F32),
            pltpu.VMEM((2, HALF, 3, 128), F32),
            pltpu.VMEM((2, HALF, 4, 128), F32),
            pltpu.VMEM((NZ, 2, 3, 128), F32),
            pltpu.VMEM((NZ, 2, 4, 128), F32),
            pltpu.VMEM((SEQS, 2, HALF, 2, 128), BF16),
            pltpu.VMEM((SEQS, 2, HALF, 4, 128), BF16),
            pltpu.VMEM((TOKENS, 2, 128), BF16),
            pltpu.VMEM((TOKENS, 4, 128), BF16),
            pltpu.VMEM((TOKENS, 2, 128), F32),
            pltpu.VMEM((TOKENS, 4, 128), F32),
            pltpu.VMEM((SEQS, PROPS, PROPS), F32),
            pltpu.VMEM((TOKENS, 6, 128), F32),
            pltpu.VMEM((TOKENS, 6, 128), BF16),
            pltpu.VMEM((TOKENS, 6, 128), BF16),
            pltpu.VMEM((TOKENS, 6, 128), F32),
            pltpu.VMEM((2, 128), BF16),
            pltpu.VMEM((NT, 8, 2, 128), BF16),
            pltpu.VMEM((TOKENS, 2, 128), F32),
            pltpu.SemaphoreType.DMA((13,)),
        ]
        + [pltpu.SemaphoreType.DMA] * 18
        + [pltpu.SemaphoreType.REGULAR] * 3,
        compiler_params=pltpu.CompilerParams(collective_id=0, has_side_effects=True),
    )(
        tokens, norm_gain.reshape(1, -1), w_query, w_key, w_value, w_out.T, lambdas, sub_gain.reshape(1, -1),
        prior, accepted, parent, key_cache, value_cache,
    )
    return pl.pallas_call(
        copy_out,
        name="copy_out",
        out_shape=tuple(jax.ShapeDtypeStruct(r.shape, r.dtype) for r in results),
        in_specs=[VMEM] * 3,
        out_specs=(HBM,) * 3,
        scratch_shapes=[pltpu.SemaphoreType.DMA((2 * SEQS + 1,))],
        compiler_params=pltpu.CompilerParams(vmem_limit_bytes=1 << 20),
    )(*results)


def solution(mesh):
    in_specs = (
        P(None, "kv"),
        P("kv"),
        P("kv", "tp"),
        P("kv", "tp"),
        P("kv", "tp"),
        P("tp", "kv"),
        P("tp"),
        P(),
        P(None, "tp", "kv", None),
        P(None, "tp", "kv", None),
        P(),
        P(),
        P(),
    )
    out_specs = (P("tp", "kv"), P(None, "tp", "kv", None), P(None, "tp", "kv", None))
    return jax.shard_map(body, mesh=mesh, in_specs=in_specs, out_specs=out_specs, check_vma=False)
```

```python
import functools

import jax
import jax.numpy as jnp
from jax import lax
from jax.experimental import pallas as pl
from jax.experimental.pallas import tpu as pltpu
from jax.sharding import PartitionSpec as P

MESH = pl.DeviceIdType.MESH
HBM = pl.BlockSpec(memory_space=pl.ANY)
VMEM = pl.BlockSpec(memory_space=pltpu.VMEM)

D = 4096
NZ, NY, NT = 16, 4, 8
HALF = NZ // 2
NEAR = NZ // 4
SEQS, PROPS, TOKENS = 4, 16, 64
EPS = 1e-06
MASKED = -1e30
HEAD_SCALE = 0.8
F32, BF16 = jnp.float32, jnp.bfloat16
LAST = (((1,), (1,)), ((), ()))
OUT = pltpu.VMEM


def z_step(k):
    odd = lax.rem(k, 2)
    return 8 + odd * lax.div(k + 1, 2) - (1 - odd) * lax.div(k, 2)


def half_step(k):
    odd = lax.rem(k, 2)
    return odd * (19 - lax.div(k, 2)) + (1 - odd) * (12 + lax.div(k, 2))


def to_plane(z, y, steps, step_of, send):
    def far(i, carry):
        send(lax.rem(z + step_of(lax.div(i, NY)), NZ), lax.rem(y + lax.rem(i, NY), NY))
        return carry

    lax.fori_loop(0, steps * NY, far, 0)

    def near(i, carry):
        send(z, lax.rem(y + i, NY))
        return carry

    lax.fori_loop(1, NY, near, 0)


def wait_bytes(ref, count, sem):
    piece = ref.at[pl.ds(0, count)]
    pltpu.make_async_copy(piece, piece, sem).wait()


def split3(x):
    high = x.astype(BF16).astype(F32)
    rest = x - high
    mid = rest.astype(BF16).astype(F32)
    return high, mid, (rest - mid).astype(BF16).astype(F32)


def fused(
    tok_in, gain_in, wq_in, wk_in, wv_in, wo_in, lam_in, sub_in, prior_in, acc_in, par_in, kc_in, vc_in,
    mixed_ref, kbuf, vbuf,
    tok, gain, wq, wk, wv, sub, par, lam, prior, acc, woall,
    part_q, part_n, yb_q, yb_n, zs_q, zs_n, zb_q, zb_n, ag_q, ag_n, ruler_q, ruler_n, rows, news, reach_ref,
    terms, csrc, cb, cterms, asrc, attb, attf,
    load_sem, y_send, y_recv, yn_send, yn_recv, w_send, w_recv, z_send, z_recv, zn_send, zn_recv,
    a_send, a_recv, an_send, an_recv, c_send, c_recv, t_send, t_recv, entered,
):
    kv, tp = lax.axis_index("kv"), lax.axis_index("tp")
    z, y = lax.div(kv, NY), lax.rem(kv, NY)
    mine = y * NZ + z
    low, upper = lax.rem(z, HALF), lax.div(z, HALF)
    length = kbuf.shape[2]

    barrier = pltpu.get_barrier_semaphore()

    def signal_z(step, sem):
        for tz in (lax.rem(z + step, NZ), lax.rem(z + NZ - step, NZ)):
            pl.semaphore_signal(sem, inc=1, device_id=(tz * NY + y, tp), device_id_type=MESH)

    for step in range(NEAR, 0, -1):
        signal_z(step, barrier)
    for i in range(1, NY):
        pl.semaphore_signal(barrier, inc=1, device_id=(z * NY + lax.rem(y + i, NY), tp), device_id_type=MESH)
    for i in range(1, NT):
        pl.semaphore_signal(barrier, inc=1, device_id=(kv, lax.rem(tp + i, NT)), device_id_type=MESH)

    pairs = (
        (tok_in, tok), (gain_in, gain), (wq_in, wq), (wk_in, wk), (wv_in, wv), (par_in, par), (wo_in, woall.at[tp]),
        (sub_in, sub), (lam_in, lam), (prior_in, prior), (acc_in, acc), (kc_in, kbuf), (vc_in, vbuf),
    )
    loads = [pltpu.make_async_copy(a, b, load_sem.at[i]) for i, (a, b) in enumerate(pairs)]
    for load in loads:
        load.start()
    for load in loads[:6]:
        load.wait()

    x = tok[...].astype(F32)
    normed = (x * gain[...]).astype(BF16)
    squares = jnp.sum(x * x, axis=1, keepdims=True)
    for w, out, c in ((wq, part_q, 0), (wk, part_n, 0), (wv, part_n, 2)):
        product = jnp.dot(normed, w[...], preferred_element_type=F32)
        out[:, c, :] = product[:, :128]
        out[:, c + 1, :] = product[:, 128:]
    part_q[:, 2, :] = jnp.broadcast_to(squares, (TOKENS, 128))

    at_i = lax.broadcasted_iota(jnp.int32, (PROPS, PROPS), 0)
    at_j = lax.broadcasted_iota(jnp.int32, (PROPS, PROPS), 1)
    for s in range(SEQS):
        reach = jnp.where((at_i == par[s : s + 1, :]) | (at_i == at_j), 1.0, 0.0)
        for _ in range(4):
            step = reach.astype(BF16)
            reach = jnp.where(jnp.dot(step, step, preferred_element_type=F32) > 0.5, 1.0, 0.0)
        reach_ref[s] = reach

    pl.semaphore_wait(barrier, 2 * NEAR + NY - 1 + NT - 1)
    signal_z(NEAR, entered)

    def send_y(part, yb, sends, recvs):
        for step in (2, 1, 3):
            ty = lax.rem(y + step, NY)
            pltpu.make_async_remote_copy(
                part.at[pl.ds(ty * NZ, NZ)], yb.at[y], sends, recvs, device_id=(z * NY + ty, tp), device_id_type=MESH
            ).start()

    def send_z(zs, zb, sends, recvs):
        def one(k, carry):
            tz = lax.rem(z + z_step(k), NZ)
            pltpu.make_async_remote_copy(
                zs.at[:, lax.rem(tz, HALF)], zb.at[z], sends, recvs, device_id=(tz * NY + y, tp), device_id_type=MESH
            ).start()
            return carry

        lax.fori_loop(0, NZ - 1, one, 0)

    def send_rows(ag, sends, recvs):
        def one(tz, ty):
            piece = ag.at[y, :, low]
            pltpu.make_async_remote_copy(
                piece, piece, sends, recvs, device_id=(tz * NY + ty, tp), device_id_type=MESH
            ).start()

        to_plane(z, y, HALF - 1, half_step, one)

    send_y(part_q, yb_q, y_send, y_recv)
    send_y(part_n, yb_n, yn_send, yn_recv)

    def send_w(i, carry):
        pltpu.make_async_remote_copy(
            woall.at[tp], woall.at[tp], w_send, w_recv, device_id=(kv, lax.rem(tp + i, NT)), device_id_type=MESH
        ).start()
        return carry

    loads[6].wait()
    lax.fori_loop(1, NT, send_w, 0)
    for load in loads[7:]:
        load.wait()

    for part, yb, recvs, zs, zb, z_sends, z_recvs in (
        (part_q, yb_q, y_recv, zs_q, zb_q, z_send, z_recv),
        (part_n, yb_n, yn_recv, zs_n, zb_n, zn_send, zn_recv),
    ):
        yb[y] = part[pl.ds(y * NZ, NZ)]
        wait_bytes(yb, NY - 1, recvs)
        zs[...] = ((yb[0] + yb[1]) + (yb[2] + yb[3])).reshape(zs.shape)
        if part is part_q:
            pl.semaphore_wait(entered, 2)
        send_z(zs, zb, z_sends, z_recvs)
        zb[z] = zs[:, low]

    wait_bytes(zb_q, NZ - 1, z_recv)
    total = jnp.sum(zb_q[...], axis=0)
    scale = lax.rsqrt(total[:, 2:3, :] / D + EPS)
    ag_q[y, :, low] = (total[:, :2, :] * scale).astype(BF16)
    send_rows(ag_q, a_send, a_recv)
    wait_bytes(zb_n, NZ - 1, zn_recv)
    ag_n[y, :, low] = (jnp.sum(zb_n[...], axis=0) * scale).astype(BF16)
    send_rows(ag_n, an_send, an_recv)

    wait_bytes(ruler_q, TOKENS - 2, a_recv)
    rows[...] = ag_q[...].astype(F32).reshape(rows.shape)
    lane = lax.broadcasted_iota(jnp.int32, (PROPS, 128), 1)
    position = lax.broadcasted_iota(jnp.int32, (2 * PROPS, length), 1) + kv * length
    for s in range(SEQS):
        settled = position < prior[s] + acc[s]
        tokens = slice(s * PROPS, (s + 1) * PROPS)
        stats = jnp.zeros((PROPS, 128), F32)
        for h in range(2):
            q = rows[tokens, h, :]
            both = jnp.concatenate([jnp.where(lane < 64, q, 0.0), jnp.where(lane < 64, 0.0, q)], axis=0).astype(BF16)
            scores = lax.dot_general(both, kbuf[s, h], LAST, preferred_element_type=F32) * 0.125
            maximum = jnp.max(jnp.where(settled, scores, MASKED), axis=1, keepdims=True)
            weight = jnp.where(settled, jnp.exp(scores - maximum), 0.0)
            totals = jnp.sum(weight, axis=1, keepdims=True)
            summed = jnp.dot(weight.astype(BF16), vbuf[s, h], preferred_element_type=F32)
            for m in range(2):
                c = 2 * m + h
                half = slice(m * PROPS, (m + 1) * PROPS)
                terms[tokens, c, :] = summed[half]
                for n, column in ((c, maximum[half]), (4 + c, totals[half])):
                    for k, piece in enumerate(split3(column)):
                        stats = jnp.where(lane == 8 * k + n, piece, stats)
        terms[tokens, 4, :] = stats
        terms[tokens, 5, :] = jnp.zeros((PROPS, 128), F32)
    csrc[...] = terms[...].astype(BF16)

    def send_c(tz, ty):
        pltpu.make_async_remote_copy(
            csrc.at[ty * NZ + tz], cb.at[mine], c_send, c_recv, device_id=(tz * NY + ty, tp), device_id_type=MESH
        ).start()

    to_plane(z, y, NZ - 1, z_step, send_c)
    cb[mine] = csrc[mine]

    wait_bytes(ruler_n, TOKENS - 2, an_recv)
    news[...] = ag_n[...].astype(F32).reshape(news.shape)
    own_q = ag_q[y, upper, low].astype(F32)
    family = pl.ds(y * PROPS, PROPS)
    related = jnp.sum(jnp.where(at_j == z, reach_ref[y], 0.0), axis=1, keepdims=True) > 0.5
    tree = []
    for m in range(2):
        for h in range(2):
            product = own_q[h : h + 1, :] * news[family, h, :]
            mine_only = lane < 64 if m == 0 else lane >= 64
            scores = jnp.sum(jnp.where(mine_only, product, 0.0), axis=1, keepdims=True) * 0.125
            maximum = jnp.max(jnp.where(related, scores, MASKED), axis=0, keepdims=True)
            weight = jnp.where(related, jnp.exp(scores - maximum), 0.0)
            summed = jnp.sum(weight.astype(BF16).astype(F32) * news[family, 2 + h, :], axis=0, keepdims=True)
            tree.append((maximum, jnp.sum(weight, axis=0, keepdims=True), summed))

    offset = lax.broadcasted_iota(jnp.int32, (length, PROPS), 0) + kv * length
    column = lax.broadcasted_iota(jnp.int32, (length, PROPS), 1)
    across = lax.broadcasted_iota(jnp.int32, (length, 128), 0) + kv * length
    for s in range(SEQS):
        end = prior[s] + acc[s]
        hot = jnp.where(offset - end == column, 1.0, 0.0).astype(BF16)
        inside = (across >= end) & (across < end + PROPS)
        for h in range(2):
            for buf, c in ((kbuf, h), (vbuf, 2 + h)):
                new = news[s * PROPS : (s + 1) * PROPS, c, :].astype(BF16)
                placed = jnp.dot(hot, new, preferred_element_type=F32)
                buf[s, h] = jnp.where(inside, placed, buf[s, h].astype(F32)).astype(BF16)

    wait_bytes(cb, NZ * NY - 1, c_recv)
    cterms[...] = cb[...].astype(F32)
    st = cterms[:, 4, :]
    heads = []
    for c in range(4):
        tree_max, tree_total, tree_summed = tree[c]
        maxima = (st[:, c : c + 1] + st[:, 8 + c : 9 + c]) + st[:, 16 + c : 17 + c]
        shares = (st[:, 4 + c : 5 + c] + st[:, 12 + c : 13 + c]) + st[:, 20 + c : 21 + c]
        largest = jnp.maximum(jnp.max(maxima, axis=0, keepdims=True), tree_max)
        factor, tree_factor = jnp.exp(maxima - largest), jnp.exp(tree_max - largest)
        whole = jnp.sum(factor * shares, axis=0, keepdims=True) + tree_factor * tree_total
        summed = jnp.sum(factor * cterms[:, c, :], axis=0, keepdims=True) + tree_factor * tree_summed
        heads.append(summed / whole)
    attended = []
    for h in range(2):
        head_out = heads[h] - lam[h] * heads[2 + h]
        square = jnp.mean(head_out * head_out, axis=1, keepdims=True)
        attended.append(head_out * lax.rsqrt(square + EPS) * sub[...] * HEAD_SCALE)
    done = jnp.concatenate(attended, axis=0).astype(BF16)
    asrc[...] = done

    target = 2 * y + upper

    def send_t(tz, ty):
        pltpu.make_async_remote_copy(
            asrc, attb.at[tp, low], t_send, t_recv, device_id=(tz * NY + ty, target), device_id_type=MESH
        ).start()

    to_plane(z, y, NZ - 1, z_step, send_t)

    @pl.when(target == tp)
    def _():
        attb[tp, low] = done
        wait_bytes(ruler_q, TOKENS - 1, t_recv)
        wait_bytes(ruler_q, TOKENS - 1, t_send)

    @pl.when(target != tp)
    def _():
        send_t(z, y)
        wait_bytes(ruler_q, TOKENS, t_recv)
        wait_bytes(ruler_q, TOKENS, t_send)

    wait_bytes(woall, NT - 1, w_recv)

    attf[...] = attb[...].astype(F32).reshape(attf.shape)
    mixed = jnp.zeros(mixed_ref.shape, F32)
    for g in range(NT):
        group = slice(g * 8, (g + 1) * 8)
        product = lax.dot_general(
            attf[group, 0, :].astype(BF16), woall[g, :, :128], LAST, preferred_element_type=F32
        ) + lax.dot_general(attf[group, 1, :].astype(BF16), woall[g, :, 128:], LAST, preferred_element_type=F32)
        mixed += product.astype(BF16).astype(F32)
    mixed_ref[...] = mixed.astype(BF16)

    wait_bytes(yb_q, NY - 1, y_send)
    wait_bytes(yb_n, NY - 1, yn_send)
    wait_bytes(woall, NT - 1, w_send)
    wait_bytes(zb_q, NZ - 1, z_send)
    wait_bytes(zb_n, NZ - 1, zn_send)
    wait_bytes(ruler_q, TOKENS - 2, a_send)
    wait_bytes(ruler_n, TOKENS - 2, an_send)
    wait_bytes(cb, NZ * NY - 1, c_send)


def copy_out(mixed_ref, k_ref, v_ref, mixed_out, k_out, v_out, sems):
    copies = [pltpu.make_async_copy(mixed_ref, mixed_out, sems.at[2 * SEQS])]
    for s in range(SEQS):
        copies.append(pltpu.make_async_copy(k_ref.at[s], k_out.at[s], sems.at[s]))
        copies.append(pltpu.make_async_copy(v_ref.at[s], v_out.at[s], sems.at[SEQS + s]))
    for copy in copies:
        copy.start()
    for copy in copies:
        copy.wait()


def body(
    tokens, norm_gain, w_query, w_key, w_value, w_out, lambdas, sub_gain, key_cache, value_cache, prior, accepted, parent
):
    length = key_cache.shape[2]
    results = pl.pallas_call(
        fused,
        name="fused",
        out_shape=(
            OUT((TOKENS // NT, 64), BF16),
            OUT(key_cache.shape, BF16),
            OUT(value_cache.shape, BF16),
        ),
        in_specs=[HBM] * 13,
        out_specs=(VMEM,) * 3,
        scratch_shapes=[
            pltpu.VMEM((TOKENS, 64), BF16),
            pltpu.VMEM((1, 64), F32),
            pltpu.VMEM((64, 256), BF16),
            pltpu.VMEM((64, 256), BF16),
            pltpu.VMEM((64, 256), BF16),
            pltpu.VMEM((1, 128), F32),
            pltpu.VMEM((SEQS, PROPS), jnp.int32),
            pltpu.SMEM((2,), F32),
            pltpu.SMEM((SEQS,), jnp.int32),
            pltpu.SMEM((SEQS,), jnp.int32),
            pltpu.VMEM((NT, 64, 256), BF16),
            pltpu.VMEM((TOKENS, 3, 128), F32),
            pltpu.VMEM((TOKENS, 4, 128), F32),
            pltpu.VMEM((NY, NZ, 3, 128), F32),
            pltpu.VMEM((NY, NZ, 4, 128), F32),
            pltpu.VMEM((2, HALF, 3, 128), F32),
            pltpu.VMEM((2, HALF, 4, 128), F32),
            pltpu.VMEM((NZ, 2, 3, 128), F32),
            pltpu.VMEM((NZ, 2, 4, 128), F32),
            pltpu.VMEM((SEQS, 2, HALF, 2, 128), BF16),
            pltpu.VMEM((SEQS, 2, HALF, 4, 128), BF16),
            pltpu.VMEM((TOKENS, 2, 128), BF16),
            pltpu.VMEM((TOKENS, 4, 128), BF16),
            pltpu.VMEM((TOKENS, 2, 128), F32),
            pltpu.VMEM((TOKENS, 4, 128), F32),
            pltpu.VMEM((SEQS, PROPS, PROPS), F32),
            pltpu.VMEM((TOKENS, 6, 128), F32),
            pltpu.VMEM((TOKENS, 6, 128), BF16),
            pltpu.VMEM((TOKENS, 6, 128), BF16),
            pltpu.VMEM((TOKENS, 6, 128), F32),
            pltpu.VMEM((2, 128), BF16),
            pltpu.VMEM((NT, 8, 2, 128), BF16),
            pltpu.VMEM((TOKENS, 2, 128), F32),
            pltpu.SemaphoreType.DMA((13,)),
        ]
        + [pltpu.SemaphoreType.DMA] * 18
        + [pltpu.SemaphoreType.REGULAR],
        compiler_params=pltpu.CompilerParams(collective_id=0, has_side_effects=True),
    )(
        tokens, norm_gain.reshape(1, -1), w_query, w_key, w_value, w_out.T, lambdas, sub_gain.reshape(1, -1),
        prior, accepted, parent, key_cache, value_cache,
    )
    return pl.pallas_call(
        copy_out,
        name="copy_out",
        out_shape=tuple(jax.ShapeDtypeStruct(r.shape, r.dtype) for r in results),
        in_specs=[VMEM] * 3,
        out_specs=(HBM,) * 3,
        scratch_shapes=[pltpu.SemaphoreType.DMA((2 * SEQS + 1,))],
        compiler_params=pltpu.CompilerParams(vmem_limit_bytes=1 << 20),
    )(*results)


def solution(mesh):
    in_specs = (
        P(None, "kv"),
        P("kv"),
        P("kv", "tp"),
        P("kv", "tp"),
        P("kv", "tp"),
        P("tp", "kv"),
        P("tp"),
        P(),
        P(None, "tp", "kv", None),
        P(None, "tp", "kv", None),
        P(),
        P(),
        P(),
    )
    out_specs = (P("tp", "kv"), P(None, "tp", "kv", None), P(None, "tp", "kv", None))
    return jax.shard_map(body, mesh=mesh, in_specs=in_specs, out_specs=out_specs, check_vma=False)
```
